32 devices in a mesh: fs: 4 (over z), tp: 4 (over y, x), rep: 2 (over core).
Axes of the slice: x: 2, y: 2, z: 4, core: 2. Of those that a mesh axis runs over, the one named last changes fastest.
Arguments:
- grads: float32 [2, 2, 8192, 2048], P('rep', None, 'fs', 'tp'), may hold values from -50 to 50
- momentum: float32 [2, 8192, 2048], P('rep', 'fs', 'tp'), may hold values from -14 to 14
Outputs:
- new_momentum: float32 [2, 8192, 2048], P('rep', 'fs', 'tp')
- step_matrix: float32 [2, 8192, 2048], P('rep', 'fs', 'tp')
The draws below stay inside these ranges and needn't reach their ends.
All inputs are finite; a program needn't handle non-finite values.
Results may differ from the reference program's by a relative error of at most 0.0003.
Values sent between devices are 32-bit elements; how exact they have to be, the bound alone decides.
A program may use at most 128 MiB of HBM per device.

```python
import math
import jax
import jax.numpy as jnp
from jax import lax

D = 2048
FF = 8192
MATS = 2
ITERS = 3
REPLICAS = 2


def region_profile(key):
    inner = jax.random.fold_in(key, 71)
    phases = jax.random.uniform(inner, (MATS, 2), jnp.float32, 0.0, 2.0 * math.pi)
    rows = jnp.arange(FF, dtype=jnp.float32) / FF
    cols = jnp.arange(D, dtype=jnp.float32) / D
    row_part = jnp.exp(0.6 * jnp.sin(2.0 * math.pi * 1.5 * rows[None, :] + phases[:, 0:1]))
    col_part = jnp.exp(0.6 * jnp.sin(2.0 * math.pi * 1.25 * cols[None, :] + phases[:, 1:2]))
    return row_part[:, :, None] * col_part[:, None, :]


def draw_grads(key, part):
    profile = region_profile(key)
    own_part = jax.random.truncated_normal(key, -4.0, 4.0, (REPLICAS, MATS, FF, D), jnp.float32)
    return own_part * profile[None]


def draw_momentum(key, part):
    profile = region_profile(key)
    inner = jax.random.fold_in(key, 29)
    return jax.random.truncated_normal(inner, -4.0, 4.0, (MATS, FF, D), jnp.float32) * profile


def setup_inputs(seed: int = 0) -> dict:
    arg_keys = jax.random.split(jax.random.key(seed), 3)
    return {
        "grads": draw_grads(jax.random.fold_in(arg_keys[2], 71), 0),
        "momentum": draw_momentum(jax.random.fold_in(arg_keys[2], 71), 0),
    }


momentum_decay = 0.95
norm_spread = 2.56
poly_linear = 3.4445
poly_cubic = -4.775
poly_quintic = 2.0315
highest = lax.Precision.HIGHEST

def orthogonalize(moment):
    squares = jnp.sum(moment * moment)
    scaling = jnp.sqrt(norm_spread * squares / D + 1.0)
    current = moment / scaling
    update = current
    for sweep in range(ITERS):
        gram = jnp.dot(current.T, current, precision=highest, preferred_element_type=jnp.float32)
        squared = jnp.dot(gram, gram, precision=highest, preferred_element_type=jnp.float32)
        factor = poly_cubic * gram + poly_quintic * squared
        update = poly_linear * current + jnp.dot(current, factor, precision=highest, preferred_element_type=jnp.float32)
        current = update
    return update * math.sqrt(FF)

def reference(grads, momentum):
    total = lax.optimization_barrier(jnp.sum(grads, axis=0))
    new_momentum = momentum_decay * momentum + total
    steps = jnp.stack([orthogonalize(new_momentum[index]) for index in range(MATS)])
    return (new_momentum, steps)
```

```python
import functools
import math

import jax
import jax.numpy as jnp
from jax import lax
from jax.experimental import pallas as pl
from jax.experimental.pallas import tpu as pltpu
from jax.sharding import PartitionSpec as P

ITERS = 3

momentum_decay = 0.95
norm_spread = 2.56
poly_linear = 3.4445
poly_cubic = -4.775
poly_quintic = 2.0315

MESH = pl.DeviceIdType.MESH
VMEM_BYTES = 63 * 1024 * 1024
SLOTS = 5


def split(value):
    high = value.astype(jnp.bfloat16)
    low = (value - high.astype(jnp.float32)).astype(jnp.bfloat16)
    return high, low


def dot3(a_high, a_low, b_high, b_low, contract=((1,), (0,))):
    def one(a, b):
        return lax.dot_general(
            a, b, (contract, ((), ())), preferred_element_type=jnp.float32
        )

    return one(a_high, b_high) + one(a_high, b_low) + one(a_low, b_high)


def bits(place):
    y = place // 2
    return place - 2 * y, y


def partner(place, s):
    x, y = bits(place)
    return (place, place + 1 - 2 * x, place + 2 - 4 * y, 3 - place)[s]


def block_row(place, chunk, slot):
    x, y = bits(place)
    if slot == 0:
        return 2 * place + chunk
    if slot == 1:
        return 2 * place + 1 - chunk
    s = slot - 1
    flip = x if s == 1 else y
    return 2 * partner(place, s) + chunk + flip - 2 * chunk * flip


def gram_kernel(x_ref, out_ref, high_ref, low_ref):
    place = lax.axis_index("tp")
    half = out_ref.shape[-1]

    @pl.when(pl.program_id(0) == 0)
    def _():
        out_ref[...] = jnp.zeros_like(out_ref)

    for q in range(x_ref.shape[0]):
        for side in range(2):
            high, low = split(x_ref[q, :, side * half : (side + 1) * half])
            high_ref[2 * q + side] = high
            low_ref[2 * q + side] = low
    for chunk in range(2):
        own = 2 * place + chunk
        for slot in range(SLOTS):
            if slot == 1 and chunk == 1:
                continue
            row = block_row(place, chunk, slot)
            out_ref[chunk, slot] += dot3(
                high_ref[row], low_ref[row], high_ref[own], low_ref[own], ((0,), (0,))
            )


def gram_share(gathered):
    count, rows, width = gathered.shape
    half = width // 2
    tile = min(rows, 512)
    return pl.pallas_call(
        gram_kernel,
        grid=(rows // tile,),
        in_specs=[pl.BlockSpec((count, tile, width), lambda i: (0, i, 0))],
        out_specs=pl.BlockSpec((2, SLOTS, half, half), lambda i: (0, 0, 0, 0)),
        out_shape=jax.ShapeDtypeStruct((2, SLOTS, half, half), jnp.float32),
        scratch_shapes=[
            pltpu.VMEM((2 * count, tile, half), jnp.bfloat16),
            pltpu.VMEM((2 * count, tile, half), jnp.bfloat16),
        ],
        compiler_params=pltpu.CompilerParams(
            vmem_limit_bytes=VMEM_BYTES, dimension_semantics=("arbitrary",)
        ),
        cost_estimate=pl.CostEstimate(
            flops=2 * 3 * 9 * rows * half * half,
            bytes_accessed=4 * rows * count * width,
            transcendentals=0,
        ),
    )(gathered)


def iterate_kernel(
    rows_count,
    share_ref,
    out_high,
    out_low,
    held,
    gram_high,
    gram_low,
    op_high,
    op_low,
    first,
    second,
    product,
    wide_high,
    wide_low,
    send_sem,
    recv_sem,
    free_sem,
):
    size = gram_high.shape[0]
    half = held.shape[-1]
    place = lax.axis_index("tp")
    neighbours = (None, partner(place, 1), partner(place, 2))
    tile = 2 * half
    tiles = size // tile

    def panel_cols(chunk):
        return pl.ds(pl.multiple_of((2 * place + chunk) * half, half), half)

    def rows_of(block, count=1):
        return pl.ds(pl.multiple_of(block * half, half), half * count)

    def eye(at):
        shape = (tile, half)
        rows = lax.broadcasted_iota(jnp.int32, shape, 0) + at * tile
        return lambda col: rows == lax.broadcasted_iota(jnp.int32, shape, 1) + col

    def copy(via, chunk, slot):
        if via == 0:
            source, target, to = held.at[0, chunk, slot], held.at[1, chunk, slot], 1
        elif via == 1:
            source, target, to = held.at[0, chunk, slot], held.at[2, chunk, slot], 2
        elif over_y(chunk, slot):
            source, target, to = held.at[1, chunk, slot], held.at[3, chunk, slot], 2
        else:
            source, target, to = held.at[2, chunk, slot], held.at[3, chunk, slot], 1
        return pltpu.make_async_remote_copy(
            src_ref=source,
            dst_ref=target,
            send_sem=send_sem.at[via, chunk, slot],
            recv_sem=recv_sem.at[via, chunk, slot],
            device_id={"tp": neighbours[to]},
            device_id_type=MESH,
        )

    def over_y(chunk, slot):
        order = [k for k in range(SLOTS) if not (chunk == 1 and k == 1)]
        place_in = order.index(slot)
        return place_in % 2 == chunk

    def slots(chunk):
        return [k for k in range(SLOTS) if not (chunk == 1 and k == 1)]

    def send(chunk, slot):
        copy(0, chunk, slot).start()
        copy(1, chunk, slot).start()

    def relay(chunk):
        for slot in slots(chunk):
            copy(0, chunk, slot).wait_recv()
            copy(1, chunk, slot).wait_recv()
            copy(2, chunk, slot).start()

    def assemble(s, chunk):
        q = partner(place, s)
        col = 2 * q + chunk
        for slot in slots(chunk):
            row = block_row(q, chunk, slot)
            value = held[s, chunk, slot]
            high, low = split(value)
            gram_high[rows_of(row), rows_of(col)] = high
            gram_low[rows_of(row), rows_of(col)] = low
            if slot > 0:
                high, low = split(value.T)
                gram_high[rows_of(col), rows_of(row)] = high
                gram_low[rows_of(col), rows_of(row)] = low

    def exchange(between):
        relay(0)
        between()
        assemble(0, 0)
        assemble(0, 1)
        for s in (1, 2):
            assemble(s, 0)
        relay(1)
        for s in (1, 2):
            assemble(s, 1)
        for chunk in range(2):
            for slot in slots(chunk):
                copy(2, chunk, slot).wait_recv()
            assemble(3, chunk)
        for via in range(3):
            for chunk in range(2):
                for slot in slots(chunk):
                    copy(via, chunk, slot).wait_send()

    def times_gram(at, count, high, low):
        rows = rows_of(at, count)
        return dot3(gram_high[rows, :], gram_low[rows, :], high, low)

    def sweep_factor(chunk, scale, also):
        def body(at, _):
            cols = panel_cols(chunk)
            rows = rows_of(2 * at, 2)
            own = gram_high[rows, cols].astype(jnp.float32) + gram_low[rows, cols].astype(
                jnp.float32
            )
            double = times_gram(2 * at, 2, gram_high[:, cols], gram_low[:, cols])
            linear = jnp.where(eye(at)((2 * place + chunk) * half), poly_linear, 0.0)
            factor = (
                linear + (poly_cubic * scale) * own + (poly_quintic * scale * scale) * double
            )
            high, low = split(factor)
            op_high[0, rows, :] = high
            op_low[0, rows, :] = low
            also(rows, factor)
            return 0

        lax.fori_loop(0, tiles, body, 0)

    def times(source, target, keep, scale):
        def body(at, _):
            rows = rows_of(2 * at, 2)
            value = scale * times_gram(2 * at, 2, op_high[source], op_low[source])
            keep[rows, :] = value
            high, low = split(value)
            op_high[target, rows, :] = high
            op_low[target, rows, :] = low
            return 0

        lax.fori_loop(0, tiles, body, 0)

    def following(chunk, scale):
        behind = None
        for slot in slots(chunk):
            row = block_row(place, chunk, slot)
            rows = rows_of(row)
            value = scale * times_gram(row, 1, op_high[0], op_low[0])
            held[0, chunk, slot] = (
                poly_linear * first[rows, :]
                + poly_cubic * second[rows, :]
                + poly_quintic * value
            )
            if behind is not None:
                send(chunk, behind)
            behind = slot
        send(chunk, behind)

    def apply(scale, finish):
        def body(at, _):
            rows = rows_of(2 * at, 2)
            part = times_gram(2 * at, 2, wide_high[0], wide_low[0])
            value = scale * part
            product[rows, :] = poly_linear * product[rows, :] + poly_cubic * value
            high, low = split(value)
            wide_high[1, rows, :] = high
            wide_low[1, rows, :] = low
            return 0

        lax.fori_loop(0, tiles, body, 0)

        def body2(at, _):
            rows = rows_of(2 * at, 2)
            part = scale * times_gram(2 * at, 2, wide_high[1], wide_low[1])
            finish(rows, product[rows, :] + poly_quintic * part)
            return 0

        lax.fori_loop(0, tiles, body2, 0)

    def keep_product(rows, value):
        product[rows, :] = value
        high, low = split(value)
        wide_high[0, rows, :] = high
        wide_low[0, rows, :] = low

    barrier = pltpu.get_barrier_semaphore()
    for to in (1, 2):
        pl.semaphore_signal(
            barrier, inc=1, device_id={"tp": neighbours[to]}, device_id_type=MESH
        )
    held[0] = share_ref[...]
    pl.semaphore_wait(barrier, 2)
    for chunk in range(2):
        for slot in slots(chunk):
            send(chunk, slot)
    exchange(lambda: None)

    on_diagonal = lax.broadcasted_iota(
        jnp.int32, (half, half), 0
    ) == lax.broadcasted_iota(jnp.int32, (half, half), 1)
    squares = jnp.zeros((1, 1), jnp.float32)
    for s in range(4):
        for chunk in range(2):
            picked = jnp.where(on_diagonal, held[s, chunk, 0], 0.0)
            squares += jnp.sum(
                jnp.sum(picked, axis=0, keepdims=True), axis=1, keepdims=True
            )
    scaling = jnp.sqrt(squares * (norm_spread / size) + 1.0)
    scale = 1.0 / (scaling * scaling)

    for sweep in range(ITERS):
        if sweep == ITERS - 1:
            last = math.sqrt(rows_count) / scaling

            def finish(rows, value):
                high, low = split(value * last)
                out_high[rows, :] = high
                out_low[rows, :] = low

            apply(scale, finish)
            break
        for to in (1, 2):
            pl.semaphore_signal(
                free_sem, inc=1, device_id={"tp": neighbours[to]}, device_id_type=MESH
            )
        for chunk in range(2):

            def also(rows, factor):
                if sweep == 0:
                    cols = slice(chunk * half, (chunk + 1) * half)
                    product[rows, cols] = factor
                    high, low = split(factor)
                    wide_high[0, rows, cols] = high
                    wide_low[0, rows, cols] = low

            sweep_factor(chunk, scale, also)
            times(0, 1, first, scale)
            times(1, 0, second, scale)
            if chunk == 0:
                pl.semaphore_wait(free_sem, 2)
            following(chunk, scale)
        if sweep == 0:
            exchange(lambda: None)
        else:
            exchange(lambda: apply(scale, keep_product))
        scale = jnp.ones((1, 1), jnp.float32)


def polynomial(share, rows_count):
    half = share.shape[-1]
    size = 8 * half
    wide = jax.ShapeDtypeStruct((size, 2 * half), jnp.bfloat16)
    return pl.pallas_call(
        functools.partial(iterate_kernel, rows_count),
        out_shape=(wide, wide),
        in_specs=[pl.BlockSpec(memory_space=pltpu.VMEM)],
        out_specs=(pl.BlockSpec(memory_space=pltpu.VMEM),) * 2,
        scratch_shapes=[
            pltpu.VMEM((4, 2, SLOTS, half, half), jnp.float32),
            pltpu.VMEM((size, size), jnp.bfloat16),
            pltpu.VMEM((size, size), jnp.bfloat16),
            pltpu.VMEM((2, size, half), jnp.bfloat16),
            pltpu.VMEM((2, size, half), jnp.bfloat16),
            pltpu.VMEM((size, half), jnp.float32),
            pltpu.VMEM((size, half), jnp.float32),
            pltpu.VMEM((size, 2 * half), jnp.float32),
            pltpu.VMEM((2, size, 2 * half), jnp.bfloat16),
            pltpu.VMEM((2, size, 2 * half), jnp.bfloat16),
            pltpu.SemaphoreType.DMA((3, 2, SLOTS)),
            pltpu.SemaphoreType.DMA((3, 2, SLOTS)),
            pltpu.SemaphoreType.REGULAR,
        ],
        compiler_params=pltpu.CompilerParams(
            collective_id=0, has_side_effects=True, vmem_limit_bytes=VMEM_BYTES
        ),
        cost_estimate=pl.CostEstimate(
            flops=2 * 3 * 12 * size * size * 2 * half,
            bytes_accessed=8 * size * 2 * half,
            transcendentals=0,
        ),
    )(share)


def step_kernel(x_ref, high_ref, low_ref, out_ref):
    width = x_ref.shape[-1]
    total = None
    for q in range(x_ref.shape[0]):
        x_high, x_low = split(x_ref[q])
        rows = slice(q * width, (q + 1) * width)
        part = dot3(x_high, x_low, high_ref[rows, :], low_ref[rows, :])
        total = part if total is None else total + part
    out_ref[...] = total


def step_of(gathered, high, low):
    count, rows, width = gathered.shape
    tile = min(rows, 256)
    whole = pl.BlockSpec((count * width, width), lambda i: (0, 0))
    return pl.pallas_call(
        step_kernel,
        grid=(rows // tile,),
        in_specs=[
            pl.BlockSpec((count, tile, width), lambda i: (0, i, 0)),
            whole,
            whole,
        ],
        out_specs=pl.BlockSpec((tile, width), lambda i: (i, 0)),
        out_shape=jax.ShapeDtypeStruct((rows, width), jnp.float32),
        compiler_params=pltpu.CompilerParams(
            vmem_limit_bytes=VMEM_BYTES, dimension_semantics=("arbitrary",)
        ),
        cost_estimate=pl.CostEstimate(
            flops=2 * 3 * rows * count * width * width,
            bytes_accessed=4 * rows * (count + 1) * width,
            transcendentals=0,
        ),
    )(gathered, high, low)


def orthogonalize(moment):
    rows_count = moment.shape[0] * lax.axis_size("fs")
    gathered = lax.all_gather(moment, "tp", axis=0, tiled=False)
    share = gram_share(gathered)
    shape = share.shape
    share = share.reshape(-1, shape[-1])
    share = lax.psum_scatter(share, "fs", scatter_dimension=0, tiled=True)
    share = lax.all_gather(share, "fs", axis=0, tiled=True).reshape(shape)
    high, low = polynomial(share, rows_count)
    return step_of(gathered, high, low)


def per_device(grads, momentum):
    shares = lax.psum_scatter(grads[0], "rep", scatter_dimension=0, tiled=True)
    moment = momentum_decay * momentum + shares
    steps = [orthogonalize(moment[k]) for k in range(moment.shape[0])]
    return (moment, jnp.stack(steps))


def solution(mesh):
    placed = (P("rep", None, "fs", "tp"), P("rep", "fs", "tp"))
    return jax.shard_map(
        per_device,
        mesh=mesh,
        in_specs=placed,
        out_specs=(P("rep", "fs", "tp"), P("rep", "fs", "tp")),
        check_vma=False,
    )
```

```python
import functools
import math

import jax
import jax.numpy as jnp
from jax import lax
from jax.experimental import pallas as pl
from jax.experimental.pallas import tpu as pltpu
from jax.sharding import PartitionSpec as P

ITERS = 3

momentum_decay = 0.95
norm_spread = 2.56
poly_linear = 3.4445
poly_cubic = -4.775
poly_quintic = 2.0315

MESH = pl.DeviceIdType.MESH
VMEM_BYTES = 63 * 1024 * 1024
SLOTS = 5
PIECES = 4


def split(value):
    high = value.astype(jnp.bfloat16)
    low = (value - high.astype(jnp.float32)).astype(jnp.bfloat16)
    return high, low


def dot3(a_high, a_low, b_high, b_low, contract=((1,), (0,))):
    def one(a, b):
        return lax.dot_general(
            a, b, (contract, ((), ())), preferred_element_type=jnp.float32
        )

    return one(a_high, b_high) + one(a_high, b_low) + one(a_low, b_high)


def bits(place):
    y = place // 2
    return place - 2 * y, y


def partner(place, s):
    x, y = bits(place)
    return (place, place + 1 - 2 * x, place + 2 - 4 * y, 3 - place)[s]


def block_row(place, chunk, slot):
    x, y = bits(place)
    if slot == 0:
        return 2 * place + chunk
    if slot == 1:
        return 2 * place + 1 - chunk
    s = slot - 1
    flip = x if s == 1 else y
    return 2 * partner(place, s) + chunk + flip - 2 * chunk * flip


def front_kernel(
    peers,
    grads_ref,
    momentum_ref,
    moment_out,
    share_out,
    high_out,
    low_out,
    grads_own,
    grads_other,
    own,
    land,
    x_high,
    x_low,
    part,
    parts,
    share,
    local_sem,
    out_sem,
    rep_send,
    rep_recv,
    x_send,
    x_recv,
    sum_send,
    sum_recv,
    all_send,
    all_recv,
):
    place = lax.axis_index("tp")
    layer = lax.axis_index("fs")
    core = lax.axis_index("rep")
    x, y = bits(place)
    neighbours = (None, partner(place, 1), partner(place, 2))
    rows, half = own.shape[1:]
    step = rows // PIECES
    slab = half // peers

    barrier = pltpu.get_barrier_semaphore()
    pl.semaphore_signal(
        barrier, inc=1, device_id={"rep": 1 - core}, device_id_type=MESH
    )
    for to in (1, 2):
        pl.semaphore_signal(
            barrier, inc=1, device_id={"tp": neighbours[to]}, device_id_type=MESH
        )

    def greet(d, _):
        pl.semaphore_signal(
            barrier,
            inc=1,
            device_id={"fs": lax.rem(layer + d, peers)},
            device_id_type=MESH,
        )
        return 0

    lax.fori_loop(1, peers, greet, 0)

    def at(piece):
        return pl.ds(piece * step, step)

    def fetch(piece):
        return pltpu.make_async_copy(
            grads_ref.at[0, core, at(piece)], grads_own.at[at(piece)], local_sem.at[piece]
        )

    def give(piece):
        return pltpu.make_async_remote_copy(
            src_ref=grads_ref.at[0, 1 - core, at(piece)],
            dst_ref=grads_other.at[at(piece)],
            send_sem=rep_send.at[piece],
            recv_sem=rep_recv.at[piece],
            device_id={"rep": 1 - core},
            device_id_type=MESH,
        )

    def copy(via, side, piece):
        if via < 2:
            source, to, lands = own, via + 1, via
            source = own.at[side, at(piece)]
        else:
            source = land.at[piece % 2, side, at(piece)]
            to, lands = 2 - piece % 2, 2
        return pltpu.make_async_remote_copy(
            src_ref=source,
            dst_ref=land.at[lands, side, at(piece)],
            send_sem=x_send.at[via, side, piece],
            recv_sem=x_recv.at[via, side, piece],
            device_id={"tp": neighbours[to]},
            device_id_type=MESH,
        )

    def send(side, piece):
        copy(0, side, piece).start()
        copy(1, side, piece).start()

    def relay(side, piece):
        copy(0, side, piece).wait_recv()
        copy(1, side, piece).wait_recv()
        copy(2, side, piece).start()

    tile = min(step, 128)

    def keep(s, side, rows_at, value):
        high, low = split(value)
        x_high[s, side, rows_at] = high
        x_low[s, side, rows_at] = low

    def divide(s, side):
        def body(k, _):
            rows_at = pl.ds(pl.multiple_of(k * tile, tile), tile)
            keep(s, side, rows_at, land[s - 1, side, rows_at])
            return 0

        lax.fori_loop(0, rows // tile, body, 0)

    def out_copies(s, side):
        return (
            pltpu.make_async_copy(
                x_high.at[s, side], high_out.at[s, side], out_sem.at[0, s, side]
            ),
            pltpu.make_async_copy(
                x_low.at[s, side], low_out.at[s, side], out_sem.at[1, s, side]
            ),
        )

    def moment_copy(side):
        return pltpu.make_async_copy(
            own.at[side],
            moment_out.at[0, :, pl.ds(side * half, half)],
            out_sem.at[2, 0, side],
        )

    def chunk_of(s, side):
        flip = x if s == 1 else y
        return side + flip - 2 * side * flip

    keys = [(0, 0, 0), (0, 1, 1), (0, 0, 1)]
    homes = [(0, 0), (1, 0), (0, 1)]
    for side in range(2):
        for s in (1, 2, 3):
            keys.append((s, side, None))
            homes.append((chunk_of(s, side), 1 + s))

    def block(key):
        s, side, chunk = keys[key]
        if s == 0:
            lhs, rhs = (0, chunk), (0, side)
        else:
            lhs, rhs = (s, side), (0, chunk_of(s, side))
        part[key] = dot3(
            x_high[lhs], x_low[lhs], x_high[rhs], x_low[rhs], ((0,), (0,))
        )

        def scatter(d, _):
            target = lax.rem(layer + d, peers)
            pltpu.make_async_remote_copy(
                src_ref=part.at[key, pl.ds(pl.multiple_of(target * slab, slab), slab)],
                dst_ref=parts.at[key, d - 1],
                send_sem=sum_send.at[key],
                recv_sem=sum_recv.at[key],
                device_id={"fs": target},
                device_id_type=MESH,
            ).start()
            return 0

        lax.fori_loop(1, peers, scatter, 0)

    def all_of(key, send_sem, recv_sem):
        return pltpu.make_async_remote_copy(
            src_ref=parts.at[key],
            dst_ref=parts.at[key],
            send_sem=send_sem.at[key],
            recv_sem=recv_sem.at[key],
            device_id={"fs": lax.rem(layer + 1, peers)},
            device_id_type=MESH,
        )

    def total(key):
        all_of(key, sum_send, sum_recv).wait_recv()
        mine = pl.ds(pl.multiple_of(layer * slab, slab), slab)
        value = part[key, mine]
        for d in range(peers - 1):
            value = value + parts[key, d]
        chunk, slot = homes[key]
        share[chunk, slot, mine] = value

        def spread(d, _):
            pltpu.make_async_remote_copy(
                src_ref=share.at[chunk, slot, mine],
                dst_ref=share.at[chunk, slot, mine],
                send_sem=all_send.at[key],
                recv_sem=all_recv.at[key],
                device_id={"fs": lax.rem(layer + d, peers)},
                device_id_type=MESH,
            ).start()
            return 0

        lax.fori_loop(1, peers, spread, 0)

    for piece in range(PIECES):
        fetch(piece).start()
    pl.semaphore_wait(barrier, 3 + peers - 1)
    for piece in range(PIECES):
        give(piece).start()
    for piece in range(PIECES):
        fetch(piece).wait()
        give(piece).wait_recv()

        def add(k, _):
            rows_at = pl.ds(pl.multiple_of(piece * step + k * tile, tile), tile)
            for side in range(2):
                cols = slice(side * half, (side + 1) * half)
                value = momentum_decay * momentum_ref[0, rows_at, cols] + (
                    grads_own[rows_at, cols] + grads_other[rows_at, cols]
                )
                own[side, rows_at] = value
                keep(0, side, rows_at, value)
            return 0

        lax.fori_loop(0, step // tile, add, 0)
        if piece > 0:
            send(0, piece - 1)
    send(0, PIECES - 1)
    send(1, 0)
    for side in range(2):
        moment_copy(side).start()
        for each in out_copies(0, side):
            each.start()
    share[1, 1] = jnp.zeros((half, half), jnp.float32)
    for key in range(3):
        block(key)
    for side in range(2):
        for piece in range(PIECES):
            relay(side, piece)
            if side == 0 and piece + 1 < PIECES:
                send(1, piece + 1)
        for s in (1, 2):
            divide(s, side)
            for each in out_copies(s, side):
                each.start()
            block(3 + 3 * side + s - 1)
        for key in (range(3) if side == 0 else (5,)):
            total(key)
        for piece in range(PIECES):
            copy(2, side, piece).wait_recv()
        divide(3, side)
        for each in out_copies(3, side):
            each.start()
        block(5 + 3 * side)
        for s in (1, 2):
            total(3 + 3 * side + s - 1)
    total(8)
    for side in range(2):
        moment_copy(side).wait()
        for s in range(4):
            for each in out_copies(s, side):
                each.wait()
        for piece in range(PIECES):
            for via in range(3):
                copy(via, side, piece).wait_send()
    for piece in range(PIECES):
        give(piece).wait_send()
    for key in range(9):
        all_of(key, sum_send, sum_recv).wait_send()
        all_of(key, all_send, all_recv).wait_send()
    for key in range(9):
        all_of(key, all_send, all_recv).wait_recv()
    share_out[...] = share[...]


def front(grads, momentum):
    peers = lax.axis_size("fs")
    _, rows, width = momentum.shape
    half = width // 2
    slab = half // peers
    parts = jax.ShapeDtypeStruct((4, 2, rows, half), jnp.bfloat16)
    anywhere = pl.BlockSpec(memory_space=pl.ANY)
    vmem = pl.BlockSpec(memory_space=pltpu.VMEM)
    semaphores = pltpu.SemaphoreType.DMA
    return pl.pallas_call(
        functools.partial(front_kernel, peers),
        out_shape=(
            jax.ShapeDtypeStruct(momentum.shape, jnp.float32),
            jax.ShapeDtypeStruct((2, SLOTS, half, half), jnp.float32),
            parts,
            parts,
        ),
        in_specs=[anywhere, vmem],
        out_specs=(anywhere, vmem, anywhere, anywhere),
        scratch_shapes=[
            pltpu.VMEM((rows, width), jnp.float32),
            pltpu.VMEM((rows, width), jnp.float32),
            pltpu.VMEM((2, rows, half), jnp.float32),
            pltpu.VMEM((3, 2, rows, half), jnp.float32),
            pltpu.VMEM((4, 2, rows, half), jnp.bfloat16),
            pltpu.VMEM((4, 2, rows, half), jnp.bfloat16),
            pltpu.VMEM((9, half, half), jnp.float32),
            pltpu.VMEM((9, peers - 1, slab, half), jnp.float32),
            pltpu.VMEM((2, SLOTS, half, half), jnp.float32),
            semaphores((PIECES,)),
            semaphores((3, 4, 2)),
            semaphores((PIECES,)),
            semaphores((PIECES,)),
            semaphores((3, 2, PIECES)),
            semaphores((3, 2, PIECES)),
            semaphores((9,)),
            semaphores((9,)),
            semaphores((9,)),
            semaphores((9,)),
        ],
        compiler_params=pltpu.CompilerParams(
            collective_id=1, has_side_effects=True, vmem_limit_bytes=VMEM_BYTES
        ),
        cost_estimate=pl.CostEstimate(
            flops=2 * 3 * 9 * rows * half * half,
            bytes_accessed=4 * rows * width * 8,
            transcendentals=0,
        ),
    )(grads, momentum)


def iterate_kernel(
    rows_count,
    share_ref,
    out_high,
    out_low,
    held,
    gram_high,
    gram_low,
    op_high,
    op_low,
    first,
    second,
    product,
    wide_high,
    wide_low,
    send_sem,
    recv_sem,
    free_sem,
):
    size = gram_high.shape[0]
    half = held.shape[-1]
    place = lax.axis_index("tp")
    neighbours = (None, partner(place, 1), partner(place, 2))
    tile = 2 * half
    tiles = size // tile

    def panel_cols(chunk):
        return pl.ds(pl.multiple_of((2 * place + chunk) * half, half), half)

    def rows_of(block, count=1):
        return pl.ds(pl.multiple_of(block * half, half), half * count)

    def eye(at):
        shape = (tile, half)
        rows = lax.broadcasted_iota(jnp.int32, shape, 0) + at * tile
        return lambda col: rows == lax.broadcasted_iota(jnp.int32, shape, 1) + col

    def copy(via, chunk, slot):
        if via == 0:
            source, target, to = held.at[0, chunk, slot], held.at[1, chunk, slot], 1
        elif via == 1:
            source, target, to = held.at[0, chunk, slot], held.at[2, chunk, slot], 2
        elif over_y(chunk, slot):
            source, target, to = held.at[1, chunk, slot], held.at[3, chunk, slot], 2
        else:
            source, target, to = held.at[2, chunk, slot], held.at[3, chunk, slot], 1
        return pltpu.make_async_remote_copy(
            src_ref=source,
            dst_ref=target,
            send_sem=send_sem.at[via, chunk, slot],
            recv_sem=recv_sem.at[via, chunk, slot],
            device_id={"tp": neighbours[to]},
            device_id_type=MESH,
        )

    def over_y(chunk, slot):
        order = [k for k in range(SLOTS) if not (chunk == 1 and k == 1)]
        place_in = order.index(slot)
        return place_in % 2 == chunk

    def slots(chunk):
        return [k for k in range(SLOTS) if not (chunk == 1 and k == 1)]

    def send(chunk, slot):
        copy(0, chunk, slot).start()
        copy(1, chunk, slot).start()

    def relay(chunk):
        for slot in slots(chunk):
            copy(0, chunk, slot).wait_recv()
            copy(1, chunk, slot).wait_recv()
            copy(2, chunk, slot).start()

    def assemble(s, chunk):
        q = partner(place, s)
        col = 2 * q + chunk
        for slot in slots(chunk):
            row = block_row(q, chunk, slot)
            value = held[s, chunk, slot]
            high, low = split(value)
            gram_high[rows_of(row), rows_of(col)] = high
            gram_low[rows_of(row), rows_of(col)] = low
            if slot > 0:
                high, low = split(value.T)
                gram_high[rows_of(col), rows_of(row)] = high
                gram_low[rows_of(col), rows_of(row)] = low

    def exchange(between):
        relay(0)
        between()
        assemble(0, 0)
        assemble(0, 1)
        for s in (1, 2):
            assemble(s, 0)
        relay(1)
        for s in (1, 2):
            assemble(s, 1)
        for chunk in range(2):
            for slot in slots(chunk):
                copy(2, chunk, slot).wait_recv()
            assemble(3, chunk)
        for via in range(3):
            for chunk in range(2):
                for slot in slots(chunk):
                    copy(via, chunk, slot).wait_send()

    def times_gram(at, count, high, low):
        rows = rows_of(at, count)
        return dot3(gram_high[rows, :], gram_low[rows, :], high, low)

    def sweep_factor(chunk, scale, also):
        def body(at, _):
            cols = panel_cols(chunk)
            rows = rows_of(2 * at, 2)
            own = gram_high[rows, cols].astype(jnp.float32) + gram_low[rows, cols].astype(
                jnp.float32
            )
            double = times_gram(2 * at, 2, gram_high[:, cols], gram_low[:, cols])
            linear = jnp.where(eye(at)((2 * place + chunk) * half), poly_linear, 0.0)
            factor = (
                linear + (poly_cubic * scale) * own + (poly_quintic * scale * scale) * double
            )
            high, low = split(factor)
            op_high[0, rows, :] = high
            op_low[0, rows, :] = low
            also(rows, factor)
            return 0

        lax.fori_loop(0, tiles, body, 0)

    def times(source, target, keep, scale):
        def body(at, _):
            rows = rows_of(2 * at, 2)
            value = scale * times_gram(2 * at, 2, op_high[source], op_low[source])
            keep[rows, :] = value
            high, low = split(value)
            op_high[target, rows, :] = high
            op_low[target, rows, :] = low
            return 0

        lax.fori_loop(0, tiles, body, 0)

    def following(chunk, scale):
        behind = None
        for slot in slots(chunk):
            row = block_row(place, chunk, slot)
            rows = rows_of(row)
            value = scale * times_gram(row, 1, op_high[0], op_low[0])
            held[0, chunk, slot] = (
                poly_linear * first[rows, :]
                + poly_cubic * second[rows, :]
                + poly_quintic * value
            )
            if behind is not None:
                send(chunk, behind)
            behind = slot
        send(chunk, behind)

    def apply(scale, finish):
        def body(at, _):
            rows = rows_of(2 * at, 2)
            part = times_gram(2 * at, 2, wide_high[0], wide_low[0])
            value = scale * part
            product[rows, :] = poly_linear * product[rows, :] + poly_cubic * value
            high, low = split(value)
            wide_high[1, rows, :] = high
            wide_low[1, rows, :] = low
            return 0

        lax.fori_loop(0, tiles, body, 0)

        def body2(at, _):
            rows = rows_of(2 * at, 2)
            part = scale * times_gram(2 * at, 2, wide_high[1], wide_low[1])
            finish(rows, product[rows, :] + poly_quintic * part)
            return 0

        lax.fori_loop(0, tiles, body2, 0)

    def keep_product(rows, value):
        product[rows, :] = value
        high, low = split(value)
        wide_high[0, rows, :] = high
        wide_low[0, rows, :] = low

    barrier = pltpu.get_barrier_semaphore()
    for to in (1, 2):
        pl.semaphore_signal(
            barrier, inc=1, device_id={"tp": neighbours[to]}, device_id_type=MESH
        )
    held[0] = share_ref[...]
    pl.semaphore_wait(barrier, 2)
    for chunk in range(2):
        for slot in slots(chunk):
            send(chunk, slot)
    exchange(lambda: None)

    on_diagonal = lax.broadcasted_iota(
        jnp.int32, (half, half), 0
    ) == lax.broadcasted_iota(jnp.int32, (half, half), 1)
    squares = jnp.zeros((1, 1), jnp.float32)
    for s in range(4):
        for chunk in range(2):
            picked = jnp.where(on_diagonal, held[s, chunk, 0], 0.0)
            squares += jnp.sum(
                jnp.sum(picked, axis=0, keepdims=True), axis=1, keepdims=True
            )
    scaling = jnp.sqrt(squares * (norm_spread / size) + 1.0)
    scale = 1.0 / (scaling * scaling)

    for sweep in range(ITERS):
        if sweep == ITERS - 1:
            last = math.sqrt(rows_count) / scaling

            def finish(rows, value):
                high, low = split(value * last)
                out_high[rows, :] = high
                out_low[rows, :] = low

            apply(scale, finish)
            break
        for to in (1, 2):
            pl.semaphore_signal(
                free_sem, inc=1, device_id={"tp": neighbours[to]}, device_id_type=MESH
            )
        for chunk in range(2):

            def also(rows, factor):
                if sweep == 0:
                    cols = slice(chunk * half, (chunk + 1) * half)
                    product[rows, cols] = factor
                    high, low = split(factor)
                    wide_high[0, rows, cols] = high
                    wide_low[0, rows, cols] = low

            sweep_factor(chunk, scale, also)
            times(0, 1, first, scale)
            times(1, 0, second, scale)
            if chunk == 0:
                pl.semaphore_wait(free_sem, 2)
            following(chunk, scale)
        if sweep == 0:
            exchange(lambda: None)
        else:
            exchange(lambda: apply(scale, keep_product))
        scale = jnp.ones((1, 1), jnp.float32)


def polynomial(share, rows_count):
    half = share.shape[-1]
    size = 8 * half
    wide = jax.ShapeDtypeStruct((size, 2 * half), jnp.bfloat16)
    return pl.pallas_call(
        functools.partial(iterate_kernel, rows_count),
        out_shape=(wide, wide),
        in_specs=[pl.BlockSpec(memory_space=pltpu.VMEM)],
        out_specs=(pl.BlockSpec(memory_space=pltpu.VMEM),) * 2,
        scratch_shapes=[
            pltpu.VMEM((4, 2, SLOTS, half, half), jnp.float32),
            pltpu.VMEM((size, size), jnp.bfloat16),
            pltpu.VMEM((size, size), jnp.bfloat16),
            pltpu.VMEM((2, size, half), jnp.bfloat16),
            pltpu.VMEM((2, size, half), jnp.bfloat16),
            pltpu.VMEM((size, half), jnp.float32),
            pltpu.VMEM((size, half), jnp.float32),
            pltpu.VMEM((size, 2 * half), jnp.float32),
            pltpu.VMEM((2, size, 2 * half), jnp.bfloat16),
            pltpu.VMEM((2, size, 2 * half), jnp.bfloat16),
            pltpu.SemaphoreType.DMA((3, 2, SLOTS)),
            pltpu.SemaphoreType.DMA((3, 2, SLOTS)),
            pltpu.SemaphoreType.REGULAR,
        ],
        compiler_params=pltpu.CompilerParams(
            collective_id=0, has_side_effects=True, vmem_limit_bytes=VMEM_BYTES
        ),
        cost_estimate=pl.CostEstimate(
            flops=2 * 3 * 12 * size * size * 2 * half,
            bytes_accessed=8 * size * 2 * half,
            transcendentals=0,
        ),
    )(share)


def step_kernel(x_high, x_low, high_ref, low_ref, out_ref):
    place = lax.axis_index("tp")
    half = x_high.shape[-1]
    total = None
    for s in range(4):
        for side in range(2):
            start = (2 * partner(place, s) + side) * half
            rows = pl.ds(pl.multiple_of(start, half), half)
            part = dot3(
                x_high[s, side], x_low[s, side], high_ref[rows, :], low_ref[rows, :]
            )
            total = part if total is None else total + part
    out_ref[0] = total


def step_of(x_high, x_low, high, low):
    count, sides, rows, half = x_high.shape
    size, width = high.shape
    tile = min(rows, 256)
    piece = pl.BlockSpec((count, sides, tile, half), lambda i: (0, 0, i, 0))
    whole = pl.BlockSpec((size, width), lambda i: (0, 0))
    return pl.pallas_call(
        step_kernel,
        grid=(rows // tile,),
        in_specs=[piece, piece, whole, whole],
        out_specs=pl.BlockSpec((1, tile, width), lambda i: (0, i, 0)),
        out_shape=jax.ShapeDtypeStruct((1, rows, width), jnp.float32),
        compiler_params=pltpu.CompilerParams(
            vmem_limit_bytes=VMEM_BYTES, dimension_semantics=("arbitrary",)
        ),
        cost_estimate=pl.CostEstimate(
            flops=2 * 3 * rows * size * width,
            bytes_accessed=4 * rows * (size + width),
            transcendentals=0,
        ),
    )(x_high, x_low, high, low)


def per_device(grads, momentum):
    rows_count = momentum.shape[1] * lax.axis_size("fs")
    moment, share, x_high, x_low = front(grads, momentum)
    high, low = polynomial(share, rows_count)
    return (moment, step_of(x_high, x_low, high, low))


def solution(mesh):
    placed = (P("rep", None, "fs", "tp"), P("rep", "fs", "tp"))
    return jax.shard_map(
        per_device,
        mesh=mesh,
        in_specs=placed,
        out_specs=(P("rep", "fs", "tp"), P("rep", "fs", "tp")),
        check_vma=False,
    )
```

```python
import functools
import math

import jax
import jax.numpy as jnp
from jax import lax
from jax.experimental import pallas as pl
from jax.experimental.pallas import tpu as pltpu
from jax.sharding import PartitionSpec as P

ITERS = 3

momentum_decay = 0.95
norm_spread = 2.56
poly_linear = 3.4445
poly_cubic = -4.775
poly_quintic = 2.0315

MESH = pl.DeviceIdType.MESH
VMEM_BYTES = 63 * 1024 * 1024
SLOTS = 5
PIECES = 4


def split(value):
    high = value.astype(jnp.bfloat16)
    low = (value - high.astype(jnp.float32)).astype(jnp.bfloat16)
    return high, low


def dot3(a_high, a_low, b_high, b_low, contract=((1,), (0,))):
    def one(a, b):
        return lax.dot_general(
            a, b, (contract, ((), ())), preferred_element_type=jnp.float32
        )

    return one(a_high, b_high) + one(a_high, b_low) + one(a_low, b_high)


def bits(place):
    y = place // 2
    return place - 2 * y, y


def partner(place, s):
    x, y = bits(place)
    return (place, place + 1 - 2 * x, place + 2 - 4 * y, 3 - place)[s]


def block_row(place, chunk, slot):
    x, y = bits(place)
    if slot == 0:
        return 2 * place + chunk
    if slot == 1:
        return 2 * place + 1 - chunk
    s = slot - 1
    flip = x if s == 1 else y
    return 2 * partner(place, s) + chunk + flip - 2 * chunk * flip


def front_kernel(
    peers,
    grads_ref,
    momentum_ref,
    moment_out,
    share_out,
    high_out,
    low_out,
    grads_own,
    grads_other,
    own,
    land,
    x_high,
    x_low,
    part,
    parts,
    share,
    local_sem,
    out_sem,
    rep_send,
    rep_recv,
    x_send,
    x_recv,
    sum_send,
    sum_recv,
    all_send,
    all_recv,
):
    place = lax.axis_index("tp")
    layer = lax.axis_index("fs")
    core = lax.axis_index("rep")
    x, y = bits(place)
    neighbours = (None, partner(place, 1), partner(place, 2))
    rows, half = own.shape[1:]
    step = rows // PIECES
    slab = half // peers

    barrier = pltpu.get_barrier_semaphore()
    pl.semaphore_signal(
        barrier, inc=1, device_id={"rep": 1 - core}, device_id_type=MESH
    )
    for to in (1, 2):
        pl.semaphore_signal(
            barrier, inc=1, device_id={"tp": neighbours[to]}, device_id_type=MESH
        )

    def greet(d, _):
        pl.semaphore_signal(
            barrier,
            inc=1,
            device_id={"fs": lax.rem(layer + d, peers)},
            device_id_type=MESH,
        )
        return 0

    lax.fori_loop(1, peers, greet, 0)

    def at(piece):
        return pl.ds(piece * step, step)

    def fetch(piece):
        return pltpu.make_async_copy(
            grads_ref.at[0, core, at(piece)], grads_own.at[at(piece)], local_sem.at[piece]
        )

    def give(piece):
        return pltpu.make_async_remote_copy(
            src_ref=grads_ref.at[0, 1 - core, at(piece)],
            dst_ref=grads_other.at[at(piece)],
            send_sem=rep_send.at[piece],
            recv_sem=rep_recv.at[piece],
            device_id={"rep": 1 - core},
            device_id_type=MESH,
        )

    def copy(via, side, piece):
        if via < 2:
            source, to, lands = own, via + 1, via
            source = own.at[side, at(piece)]
        else:
            source = land.at[piece % 2, side, at(piece)]
            to, lands = 2 - piece % 2, 2
        return pltpu.make_async_remote_copy(
            src_ref=source,
            dst_ref=land.at[lands, side, at(piece)],
            send_sem=x_send.at[via, side, piece],
            recv_sem=x_recv.at[via, side, piece],
            device_id={"tp": neighbours[to]},
            device_id_type=MESH,
        )

    def send(side, piece):
        copy(0, side, piece).start()
        copy(1, side, piece).start()

    def relay(side, piece):
        copy(0, side, piece).wait_recv()
        copy(1, side, piece).wait_recv()
        copy(2, side, piece).start()

    tile = min(step, 128)

    def keep(s, side, rows_at, value):
        high, low = split(value)
        x_high[s, side, rows_at] = high
        x_low[s, side, rows_at] = low

    def divide(s, side):
        def body(k, _):
            rows_at = pl.ds(pl.multiple_of(k * tile, tile), tile)
            keep(s, side, rows_at, land[s - 1, side, rows_at])
            return 0

        lax.fori_loop(0, rows // tile, body, 0)

    def out_copies(s, side):
        return (
            pltpu.make_async_copy(
                x_high.at[s, side], high_out.at[s, side], out_sem.at[0, s, side]
            ),
            pltpu.make_async_copy(
                x_low.at[s, side], low_out.at[s, side], out_sem.at[1, s, side]
            ),
        )

    def moment_copy(side):
        return pltpu.make_async_copy(
            own.at[side],
            moment_out.at[0, :, pl.ds(side * half, half)],
            out_sem.at[2, 0, side],
        )

    def chunk_of(s, side):
        flip = x if s == 1 else y
        return side + flip - 2 * side * flip

    keys = [(0, 0, 0), (0, 1, 1), (0, 0, 1)]
    homes = [(0, 0), (1, 0), (0, 1)]
    for side in range(2):
        for s in (1, 2, 3):
            keys.append((s, side, None))
            homes.append((chunk_of(s, side), 1 + s))

    def block(key):
        s, side, chunk = keys[key]
        if s == 0:
            lhs, rhs = (0, chunk), (0, side)
        else:
            lhs, rhs = (s, side), (0, chunk_of(s, side))
        part[key] = dot3(
            x_high[lhs], x_low[lhs], x_high[rhs], x_low[rhs], ((0,), (0,))
        )

        def scatter(d, _):
            target = lax.rem(layer + d, peers)
            pltpu.make_async_remote_copy(
                src_ref=part.at[key, pl.ds(pl.multiple_of(target * slab, slab), slab)],
                dst_ref=parts.at[key, d - 1],
                send_sem=sum_send.at[key],
                recv_sem=sum_recv.at[key],
                device_id={"fs": target},
                device_id_type=MESH,
            ).start()
            return 0

        lax.fori_loop(1, peers, scatter, 0)

    def all_of(key, send_sem, recv_sem):
        return pltpu.make_async_remote_copy(
            src_ref=parts.at[key],
            dst_ref=parts.at[key],
            send_sem=send_sem.at[key],
            recv_sem=recv_sem.at[key],
            device_id={"fs": lax.rem(layer + 1, peers)},
            device_id_type=MESH,
        )

    def total(key):
        all_of(key, sum_send, sum_recv).wait_recv()
        mine = pl.ds(pl.multiple_of(layer * slab, slab), slab)
        value = part[key, mine]
        for d in range(peers - 1):
            value = value + parts[key, d]
        chunk, slot = homes[key]
        share[chunk, slot, mine] = value

        def spread(d, _):
            pltpu.make_async_remote_copy(
                src_ref=share.at[chunk, slot, mine],
                dst_ref=share.at[chunk, slot, mine],
                send_sem=all_send.at[key],
                recv_sem=all_recv.at[key],
                device_id={"fs": lax.rem(layer + d, peers)},
                device_id_type=MESH,
            ).start()
            return 0

        lax.fori_loop(1, peers, spread, 0)

    for piece in range(PIECES):
        fetch(piece).start()
    pl.semaphore_wait(barrier, 3 + peers - 1)
    for piece in range(PIECES):
        give(piece).start()
    for piece in range(PIECES):
        fetch(piece).wait()
        give(piece).wait_recv()

        def add(k, _):
            rows_at = pl.ds(pl.multiple_of(piece * step + k * tile, tile), tile)
            for side in range(2):
                cols = slice(side * half, (side + 1) * half)
                value = momentum_decay * momentum_ref[0, rows_at, cols] + (
                    grads_own[rows_at, cols] + grads_other[rows_at, cols]
                )
                own[side, rows_at] = value
                keep(0, side, rows_at, value)
            return 0

        lax.fori_loop(0, step // tile, add, 0)
        if piece > 0:
            send(0, piece - 1)
    send(0, PIECES - 1)
    send(1, 0)
    for side in range(2):
        moment_copy(side).start()
        for each in out_copies(0, side):
            each.start()
    share[1, 1] = jnp.zeros((half, half), jnp.float32)
    for key in range(3):
        block(key)
    for side in range(2):
        for piece in range(PIECES):
            relay(side, piece)
            if side == 0 and piece + 1 < PIECES:
                send(1, piece + 1)
        for s in (1, 2):
            divide(s, side)
            for each in out_copies(s, side):
                each.start()
            block(3 + 3 * side + s - 1)
        for key in (range(3) if side == 0 else (5,)):
            total(key)
        for piece in range(PIECES):
            copy(2, side, piece).wait_recv()
        divide(3, side)
        for each in out_copies(3, side):
            each.start()
        block(5 + 3 * side)
        for s in (1, 2):
            total(3 + 3 * side + s - 1)
    total(8)
    for side in range(2):
        moment_copy(side).wait()
        for s in range(4):
            for each in out_copies(s, side):
                each.wait()
        for piece in range(PIECES):
            for via in range(3):
                copy(via, side, piece).wait_send()
    for piece in range(PIECES):
        give(piece).wait_send()
    for key in range(9):
        all_of(key, sum_send, sum_recv).wait_send()
        all_of(key, all_send, all_recv).wait_send()
    for key in range(9):
        all_of(key, all_send, all_recv).wait_recv()
    share_out[...] = share[...]


def front(grads, momentum):
    peers = lax.axis_size("fs")
    _, rows, width = momentum.shape
    half = width // 2
    slab = half // peers
    parts = jax.ShapeDtypeStruct((4, 2, rows, half), jnp.bfloat16)
    anywhere = pl.BlockSpec(memory_space=pl.ANY)
    vmem = pl.BlockSpec(memory_space=pltpu.VMEM)
    semaphores = pltpu.SemaphoreType.DMA
    return pl.pallas_call(
        functools.partial(front_kernel, peers),
        out_shape=(
            jax.ShapeDtypeStruct(momentum.shape, jnp.float32),
            jax.ShapeDtypeStruct((2, SLOTS, half, half), jnp.float32),
            parts,
            parts,
        ),
        in_specs=[anywhere, vmem],
        out_specs=(anywhere, vmem, anywhere, anywhere),
        scratch_shapes=[
            pltpu.VMEM((rows, width), jnp.float32),
            pltpu.VMEM((rows, width), jnp.float32),
            pltpu.VMEM((2, rows, half), jnp.float32),
            pltpu.VMEM((3, 2, rows, half), jnp.float32),
            pltpu.VMEM((4, 2, rows, half), jnp.bfloat16),
            pltpu.VMEM((4, 2, rows, half), jnp.bfloat16),
            pltpu.VMEM((9, half, half), jnp.float32),
            pltpu.VMEM((9, peers - 1, slab, half), jnp.float32),
            pltpu.VMEM((2, SLOTS, half, half), jnp.float32),
            semaphores((PIECES,)),
            semaphores((3, 4, 2)),
            semaphores((PIECES,)),
            semaphores((PIECES,)),
            semaphores((3, 2, PIECES)),
            semaphores((3, 2, PIECES)),
            semaphores((9,)),
            semaphores((9,)),
            semaphores((9,)),
            semaphores((9,)),
        ],
        compiler_params=pltpu.CompilerParams(
            collective_id=1, has_side_effects=True, vmem_limit_bytes=VMEM_BYTES
        ),
        cost_estimate=pl.CostEstimate(
            flops=2 * 3 * 9 * rows * half * half,
            bytes_accessed=4 * rows * width * 8,
            transcendentals=0,
        ),
    )(grads, momentum)


def iterate_kernel(
    rows_count,
    share_ref,
    out_high,
    out_low,
    held,
    gram_high,
    gram_low,
    op_high,
    op_low,
    first,
    second,
    product,
    wide_high,
    wide_low,
    send_sem,
    recv_sem,
    free_sem,
):
    size = gram_high.shape[0]
    half = held.shape[-1]
    place = lax.axis_index("tp")
    neighbours = (None, partner(place, 1), partner(place, 2))
    tile = 2 * half
    tiles = size // tile

    def panel_cols(chunk):
        return pl.ds(pl.multiple_of((2 * place + chunk) * half, half), half)

    def rows_of(block, count=1):
        return pl.ds(pl.multiple_of(block * half, half), half * count)

    def eye(at):
        shape = (tile, half)
        rows = lax.broadcasted_iota(jnp.int32, shape, 0) + at * tile
        return lambda col: rows == lax.broadcasted_iota(jnp.int32, shape, 1) + col

    layer = lax.axis_index("fs")
    odd = lax.rem(layer, 2)
    twin = layer + 1 - 2 * odd

    def turn(chunk, slot):
        return lax.rem(odd + slots(chunk).index(slot) + chunk, 2)

    def slots(chunk):
        return [k for k in range(SLOTS) if not (chunk == 1 and k == 1)]

    def beside(way):
        return (1 - way) * neighbours[1] + way * neighbours[2]

    def copy(via, chunk, slot):
        way = turn(chunk, slot)
        if via == 0:
            source, target = held.at[0, chunk, slot], held.at[1 + way, chunk, slot]
        elif via == 1:
            source, target = held.at[1 + way, chunk, slot], held.at[3, chunk, slot]
        else:
            source = target = held.at[1 + way, chunk, slot]
        return pltpu.make_async_remote_copy(
            src_ref=source,
            dst_ref=target,
            send_sem=send_sem.at[via, chunk, slot],
            recv_sem=recv_sem.at[via, chunk, slot],
            device_id={"fs": twin}
            if via == 2
            else {"tp": beside(way if via == 0 else 1 - way)},
            device_id_type=MESH,
        )

    def send(chunk, slot):
        copy(0, chunk, slot).start()

    def relay(chunk, slot):
        copy(0, chunk, slot).wait_recv()
        copy(1, chunk, slot).start()
        copy(2, chunk, slot).start()

    x, y = bits(place)

    def place_block(s, chunk, slot):
        across_y = s // 2
        across_x = s - 2 * across_y
        q = place + across_x * (1 - 2 * x) + across_y * (2 - 4 * y)
        col = 2 * q + chunk
        row = block_row(q, chunk, slot)
        value = held[s, chunk, slot]
        high, low = split(value)
        gram_high[rows_of(row), rows_of(col)] = high
        gram_low[rows_of(row), rows_of(col)] = low
        if slot > 0:
            high, low = split(value.T)
            gram_high[rows_of(col), rows_of(row)] = high
            gram_low[rows_of(col), rows_of(row)] = low

    def arrived(chunk, slot):
        copy(1, chunk, slot).wait_recv()
        copy(2, chunk, slot).wait_recv()

    def exchange(between):
        between()

        def place_all(first_source, chunk, slot):
            def body(s, _):
                place_block(s, chunk, slot)
                return 0

            lax.fori_loop(first_source, 4, body, 0)

        for slot in slots(0):
            arrived(0, slot)
            place_all(0, 0, slot)
        for slot in slots(1):
            arrived(1, slot)
            place_all(0, 1, slot)
        for via in range(3):
            for chunk in range(2):
                for slot in slots(chunk):
                    copy(via, chunk, slot).wait_send()

    def times_gram(at, count, high, low):
        rows = rows_of(at, count)
        return dot3(gram_high[rows, :], gram_low[rows, :], high, low)

    def sweep_factor(chunk, scale, also):
        def body(at, _):
            cols = panel_cols(chunk)
            rows = rows_of(2 * at, 2)
            own = gram_high[rows, cols].astype(jnp.float32) + gram_low[rows, cols].astype(
                jnp.float32
            )
            double = times_gram(2 * at, 2, gram_high[:, cols], gram_low[:, cols])
            linear = jnp.where(eye(at)((2 * place + chunk) * half), poly_linear, 0.0)
            factor = (
                linear + (poly_cubic * scale) * own + (poly_quintic * scale * scale) * double
            )
            high, low = split(factor)
            op_high[0, rows, :] = high
            op_low[0, rows, :] = low
            also(rows, factor)
            return 0

        lax.fori_loop(0, tiles, body, 0)

    def times(source, target, keep, scale):
        def body(at, _):
            rows = rows_of(2 * at, 2)
            value = scale * times_gram(2 * at, 2, op_high[source], op_low[source])
            keep[rows, :] = value
            high, low = split(value)
            op_high[target, rows, :] = high
            op_low[target, rows, :] = low
            return 0

        lax.fori_loop(0, tiles, body, 0)

    def following(chunk, scale):
        order = slots(chunk)
        blocks = [block_row(place, chunk, slot) for slot in order]

        def body(at, _):
            row = sum(jnp.where(at == k, blocks[k], 0) for k in range(len(order)))
            slot = sum(jnp.where(at == k, order[k], 0) for k in range(len(order)))
            rows = rows_of(row)
            value = scale * times_gram(row, 1, op_high[0], op_low[0])
            held[0, chunk, slot] = (
                poly_linear * first[rows, :]
                + poly_cubic * second[rows, :]
                + poly_quintic * value
            )
            for k in range(len(order) - 1):

                @pl.when(at == k + 1)
                def _():
                    send(chunk, order[k])

            return 0

        lax.fori_loop(0, len(order), body, 0)
        send(chunk, order[-1])

    def relay_last():
        for slot in slots(1):
            relay(1, slot)

    def apply(scale, finish, between=lambda: None):
        def body(at, _):
            rows = rows_of(2 * at, 2)
            part = times_gram(2 * at, 2, wide_high[0], wide_low[0])
            value = scale * part
            product[rows, :] = poly_linear * product[rows, :] + poly_cubic * value
            high, low = split(value)
            wide_high[1, rows, :] = high
            wide_low[1, rows, :] = low
            return 0

        lax.fori_loop(0, tiles, body, 0)
        between()

        def body2(at, _):
            rows = rows_of(2 * at, 2)
            part = scale * times_gram(2 * at, 2, wide_high[1], wide_low[1])
            finish(rows, product[rows, :] + poly_quintic * part)
            return 0

        lax.fori_loop(0, tiles, body2, 0)

    def keep_product(rows, value):
        product[rows, :] = value
        high, low = split(value)
        wide_high[0, rows, :] = high
        wide_low[0, rows, :] = low

    barrier = pltpu.get_barrier_semaphore()
    def tell(semaphore):
        for to in (1, 2):
            pl.semaphore_signal(
                semaphore, inc=1, device_id={"tp": neighbours[to]}, device_id_type=MESH
            )
        pl.semaphore_signal(
            semaphore, inc=1, device_id={"fs": twin}, device_id_type=MESH
        )

    tell(barrier)
    held[0] = share_ref[...]
    pl.semaphore_wait(barrier, 3)
    for chunk in range(2):
        for slot in slots(chunk):
            send(chunk, slot)
    for slot in slots(0):
        relay(0, slot)
    relay_last()
    exchange(lambda: None)

    on_diagonal = lax.broadcasted_iota(
        jnp.int32, (half, half), 0
    ) == lax.broadcasted_iota(jnp.int32, (half, half), 1)
    squares = jnp.zeros((1, 1), jnp.float32)
    for s in range(4):
        for chunk in range(2):
            picked = jnp.where(on_diagonal, held[s, chunk, 0], 0.0)
            squares += jnp.sum(
                jnp.sum(picked, axis=0, keepdims=True), axis=1, keepdims=True
            )
    scaling = jnp.sqrt(squares * (norm_spread / size) + 1.0)
    scale = 1.0 / (scaling * scaling)

    for sweep in range(ITERS):
        if sweep == ITERS - 1:
            last = math.sqrt(rows_count) / scaling

            def finish(rows, value):
                high, low = split(value * last)
                out_high[rows, :] = high
                out_low[rows, :] = low

            apply(scale, finish)
            break
        tell(free_sem)
        for chunk in range(2):

            def also(rows, factor):
                if sweep == 0:
                    cols = slice(chunk * half, (chunk + 1) * half)
                    product[rows, cols] = factor
                    high, low = split(factor)
                    wide_high[0, rows, cols] = high
                    wide_low[0, rows, cols] = low

            sweep_factor(chunk, scale, also)
            if chunk == 1:
                relay(0, 0)
            times(0, 1, first, scale)
            if chunk == 1:
                relay(0, 1)
                relay(0, 2)
            times(1, 0, second, scale)
            if chunk == 1:
                relay(0, 3)
                relay(0, 4)
            if chunk == 0:
                pl.semaphore_wait(free_sem, 3)
            following(chunk, scale)
        if sweep == 0:
            relay_last()
            exchange(lambda: None)
        else:
            exchange(lambda: apply(scale, keep_product, relay_last))
        scale = jnp.ones((1, 1), jnp.float32)


def polynomial(share, rows_count):
    half = share.shape[-1]
    size = 8 * half
    wide = jax.ShapeDtypeStruct((size, 2 * half), jnp.bfloat16)
    return pl.pallas_call(
        functools.partial(iterate_kernel, rows_count),
        out_shape=(wide, wide),
        in_specs=[pl.BlockSpec(memory_space=pltpu.VMEM)],
        out_specs=(pl.BlockSpec(memory_space=pltpu.VMEM),) * 2,
        scratch_shapes=[
            pltpu.VMEM((4, 2, SLOTS, half, half), jnp.float32),
            pltpu.VMEM((size, size), jnp.bfloat16),
            pltpu.VMEM((size, size), jnp.bfloat16),
            pltpu.VMEM((2, size, half), jnp.bfloat16),
            pltpu.VMEM((2, size, half), jnp.bfloat16),
            pltpu.VMEM((size, half), jnp.float32),
            pltpu.VMEM((size, half), jnp.float32),
            pltpu.VMEM((size, 2 * half), jnp.float32),
            pltpu.VMEM((2, size, 2 * half), jnp.bfloat16),
            pltpu.VMEM((2, size, 2 * half), jnp.bfloat16),
            pltpu.SemaphoreType.DMA((3, 2, SLOTS)),
            pltpu.SemaphoreType.DMA((3, 2, SLOTS)),
            pltpu.SemaphoreType.REGULAR,
        ],
        compiler_params=pltpu.CompilerParams(
            collective_id=0, has_side_effects=True, vmem_limit_bytes=VMEM_BYTES
        ),
        cost_estimate=pl.CostEstimate(
            flops=2 * 3 * 12 * size * size * 2 * half,
            bytes_accessed=8 * size * 2 * half,
            transcendentals=0,
        ),
    )(share)


def step_kernel(x_high, x_low, high_ref, low_ref, out_ref):
    place = lax.axis_index("tp")
    half = x_high.shape[-1]
    total = None
    for s in range(4):
        for side in range(2):
            start = (2 * partner(place, s) + side) * half
            rows = pl.ds(pl.multiple_of(start, half), half)
            part = dot3(
                x_high[s, side], x_low[s, side], high_ref[rows, :], low_ref[rows, :]
            )
            total = part if total is None else total + part
    out_ref[0] = total


def step_of(x_high, x_low, high, low):
    count, sides, rows, half = x_high.shape
    size, width = high.shape
    tile = min(rows, 256)
    piece = pl.BlockSpec((count, sides, tile, half), lambda i: (0, 0, i, 0))
    whole = pl.BlockSpec((size, width), lambda i: (0, 0))
    return pl.pallas_call(
        step_kernel,
        grid=(rows // tile,),
        in_specs=[piece, piece, whole, whole],
        out_specs=pl.BlockSpec((1, tile, width), lambda i: (0, i, 0)),
        out_shape=jax.ShapeDtypeStruct((1, rows, width), jnp.float32),
        compiler_params=pltpu.CompilerParams(
            vmem_limit_bytes=VMEM_BYTES, dimension_semantics=("arbitrary",)
        ),
        cost_estimate=pl.CostEstimate(
            flops=2 * 3 * rows * size * width,
            bytes_accessed=4 * rows * (size + width),
            transcendentals=0,
        ),
    )(x_high, x_low, high, low)


def per_device(grads, momentum):
    rows_count = momentum.shape[1] * lax.axis_size("fs")
    moment, share, x_high, x_low = front(grads, momentum)
    high, low = polynomial(share, rows_count)
    return (moment, step_of(x_high, x_low, high, low))


def solution(mesh):
    placed = (P("rep", None, "fs", "tp"), P("rep", "fs", "tp"))
    return jax.shard_map(
        per_device,
        mesh=mesh,
        in_specs=placed,
        out_specs=(P("rep", "fs", "tp"), P("rep", "fs", "tp")),
        check_vma=False,
    )
```
